32 devices in a mesh: ep: 8 (over z, x), tp: 4 (over y, core).
Axes of the slice: x: 2, y: 2, z: 4, core: 2. Of those that a mesh axis runs over, the one named last changes fastest.
Arguments:
- query_rows: bfloat16 [1024, 1024], P('ep', 'tp'), may hold values from -6 to 6
- key_rows: bfloat16 [1024, 256], P('ep', 'tp'), may hold values from -6 to 6
- retrieved_vector_table: bfloat16 [1024, 256], P('ep', 'tp'), may hold values from -6 to 6
- key_bias: bfloat16 [1024, 4], P('ep', 'tp'), may hold values from -1.5 to 12
- score_offset: float32 [16], P('tp'), may hold values from 3 to 12
- out_weight: bfloat16 [1024, 2048], P('tp'), may hold values from -0.1875 to 0.1875
- second_batch_activations: bfloat16 [1024, 2048], P('ep'), may hold values from -6 to 6
- norm_gain: float32 [2048], replicated, may hold values from 0.1 to 1.9
- expert_index: int32 [1024, 2], P('ep'), may hold values from 0 to 7, all different within a row; in each aligned block of 128 rows (0 to 127, 128 to 255, ...) at most 64 rows name the same one
- route_weight: float32 [1024, 2], P('ep'), may hold values from 0.2 to 1
- gate_weight: bfloat16 [8, 2048, 1024], P('ep', None, 'tp'), may hold values from -0.125 to 0.125
- up_weight: bfloat16 [8, 2048, 1024], P('ep', None, 'tp'), may hold values from -0.125 to 0.125
- down_weight: bfloat16 [8, 1024, 2048], P('ep', 'tp'), may hold values from -0.1875 to 0.1875
Outputs:
- attention_out: bfloat16 [1024, 2048], P(('ep', 'tp'))
- expert_out: bfloat16 [1024, 2048], P('ep', 'tp')
The draws below stay inside these ranges and needn't reach their ends.
Inputs may be any that keep to these rules, and one draw needn't show every extreme that they name: `expert_index`: each row names 2 different experts; in each aligned block of 128 rows (the rows of one index of ep) no expert is named by more than 64 rows, a bound that some block reaches.
All inputs are finite; a program needn't handle non-finite values.
Results may differ from the reference program's by a relative error of at most 0.011.
Values may be sent and summed in bfloat16 or wider, within the bound.
A program may use at most 64 MiB of HBM per device.

```python
import math
import jax
import jax.numpy as jnp
import numpy as np
from jax import lax

D = 2048
HEADS = 16
KVH = 4
HD = 64
FF = 1024
TOP = 2
SEQS = 1
ROWS_A = 128
TOK_B = 128
EXPERTS = 8
CAP = 64
LENGTH = 1024
TOKENS_A = 1024
TOKENS_B = 1024
N_EP = 8
N_TP = 4


def draw_score_offset(key, part):
    slow_key, fast_key, pick_key = jax.random.split(jax.random.fold_in(key, 11), 3)
    base = max(math.log(LENGTH) - 0.5, 3.5)
    slow = base + jax.random.uniform(slow_key, (HEADS,), jnp.float32, 0.0, 1.0)
    fast = 3.0 + jax.random.uniform(fast_key, (HEADS,), jnp.float32, 0.0, 0.8)
    share = 0.5
    slow_heads = jax.random.uniform(pick_key, (HEADS,), jnp.float32) < share
    return jnp.where(slow_heads, slow, fast).astype(jnp.float32)


def draw_key_bias(key, part):
    block_key, spot_key, size_key = jax.random.split(jax.random.fold_in(key, 23), 3)
    blocks = TOKENS_A // ROWS_A
    reach = 1.0
    block_level = jax.random.uniform(block_key, (blocks, 1, KVH), jnp.float32, -reach, reach)
    block_level = jnp.broadcast_to(block_level, (blocks, ROWS_A, KVH)).reshape(TOKENS_A, KVH)
    spots = jax.random.randint(spot_key, (SEQS, 3), 0, LENGTH)
    starts = jnp.arange(SEQS, dtype=jnp.int32)[:, None] * LENGTH
    flagged_entries = (starts + spots).reshape(-1)
    position_index = jnp.arange(TOKENS_A, dtype=jnp.int32)
    flagged_rows = jnp.any(position_index[:, None] == flagged_entries[None, :], axis=1)
    spot_logit = math.log(LENGTH) + jax.random.uniform(size_key, (TOKENS_A, KVH), jnp.float32, -1.0, 0.5)
    return jnp.where(flagged_rows[:, None], spot_logit, block_level).astype(jnp.bfloat16)


def block_scale(key, shape, shards, smallest, top_value):
    level, own = 1.0, jax.random.fold_in(key, 6)
    for dim, blocks in shards:
        steps = jnp.exp(jax.random.uniform(jax.random.fold_in(own, dim), (blocks,), jnp.float32, smallest / len(shards), top_value / len(shards)))
        level = level * jnp.repeat(steps, shape[dim] // blocks).reshape([-1 if axis == dim else 1 for axis in range(len(shape))])
    return level


def routed_block(own_key, own, number, rows, amount, top, most, skew):
    ranking = jax.random.permutation(own_key, amount)
    packed, usual = portions_of(amount, rows * top, most, skew, True), portions_of(amount, rows * top, most, skew, False)
    places = jnp.arange(amount)

    def named(tallies, rotation):
        used = int((tallies > 0).sum())
        fixed = max(1, used // 4)
        shifted = fixed + (places - fixed + rotation * (used - fixed)) % max(1, amount - fixed)
        return jnp.zeros((amount,), jnp.int32).at[ranking[jnp.where(places < fixed, places, shifted)]].set(jnp.asarray(tallies, jnp.int32))

    tallies = jnp.where(number % 4 == 0, named(packed, number // 4), named(usual, number - number // 4 - 1))
    mixed = jax.random.permutation(jax.random.fold_in(own, 3), amount)
    source_of, receiver = mixed[0:amount // 2 * 2:2], mixed[1:amount // 2 * 2:2]
    room = jnp.minimum(tallies[source_of] - 1, most - tallies[receiver]) // 2
    room = jnp.where((source_of == ranking[0]) | (receiver == ranking[0]) | (tallies[receiver] == 0), 0, jnp.maximum(room, 0))
    shifted = jax.random.randint(jax.random.fold_in(own, 4), (amount // 2,), 0, 1 << 20) % (room + 1)
    tallies = tallies.at[source_of].add(-shifted).at[receiver].add(shifted)
    items = jnp.searchsorted(jnp.cumsum(tallies), jnp.arange(rows * top), side="right").astype(jnp.int32)
    listing = items.reshape(top, rows).T
    listing = listing[jax.random.permutation(jax.random.fold_in(own, 1), rows)]
    rotation = jax.random.randint(jax.random.fold_in(own, 2), (rows, 1), 0, top)
    return jnp.take_along_axis(listing, (jnp.arange(top)[None, :] + rotation) % top, axis=1)


def portions_of(number_of, total, bound, skew, full):
    loads = [(1 << 20) // math.isqrt(standing ** skew) + 1 for standing in range(1, number_of + 1)]
    largest = bound if full else min(bound, max(-(-total // number_of), total * loads[0] // sum(loads)))
    least = 1 if total - largest >= number_of - 1 else 0
    holding, spare = [largest] + [least] * (number_of - 1), total - largest - least * (number_of - 1)
    while spare > 0:
        free = [i for i in range(1, number_of) if holding[i] < largest] or [i for i in range(1, number_of) if holding[i] < bound]
        whole, budget = sum([loads[i] for i in free]), spare
        for i in free:
            extra = min(bound - holding[i], max(1, budget * loads[i] // whole), spare)
            holding[i] = holding[i] + extra
            spare = spare - extra
    return np.array(holding)


def centred(own_key, extent, scale, most, cuts=(), kind=jnp.bfloat16):
    values = scale * jax.random.normal(own_key, extent, jnp.float32)
    if cuts:
        values = values * block_scale(own_key, extent, cuts, -0.22, 0.18)
    return jnp.clip(values, -most, most).astype(kind)


def setup_inputs(seed: int = 0) -> dict:
    key_of = jax.random.split(jax.random.key(seed), 14)
    query_rows = centred(key_of[0], (TOKENS_A, HEADS * HD), 1.0, 6.0, ((0, 8), (1, 4)))
    key_rows = centred(key_of[1], (TOKENS_A, KVH * HD), 1.0, 6.0, ((0, 8), (1, 4)))
    retrieved_vector_table = centred(key_of[2], (TOKENS_A, KVH * HD), 1.0, 6.0, ((0, 8), (1, 4)))
    key_bias = draw_key_bias(jax.random.fold_in(key_of[13], 71), 0)
    score_offset = draw_score_offset(jax.random.fold_in(key_of[13], 71), 0)
    out_weight = centred(key_of[5], (HEADS * HD, D), (HEADS * HD) ** -0.5, 0.1875, ((0, 4),))
    second_batch_activations = centred(key_of[6], (TOKENS_B, D), 1.0, 6.0, ((0, 8),))
    norm_gain = jnp.clip(1.0 + 0.18 * jax.random.normal(key_of[7], (D,), jnp.float32), 0.1, 1.9)
    expert_index_keys = jax.random.split(jax.random.fold_in(key_of[8], 1), TOKENS_B // TOK_B)
    expert_index_turns = jax.random.permutation(jax.random.fold_in(key_of[8], 3), TOKENS_B // TOK_B)
    expert_index = jax.vmap(lambda own, number: routed_block(jax.random.fold_in(key_of[8], 2), own, number, TOK_B, EXPERTS, TOP, CAP, 2))(expert_index_keys, expert_index_turns).reshape((TOKENS_B, TOP))
    route_weight = jnp.clip(0.2 + 0.8 * jax.random.uniform(key_of[9], (TOKENS_B, TOP), jnp.float32) ** block_scale(key_of[9], (TOKENS_B, TOP), ((0, 8),), -0.2, 0.2), 0.2, 1.0)
    gate_weight = centred(key_of[10], (EXPERTS, D, FF), D ** -0.5, 0.125, ((0, 8), (2, 4)))
    up_weight = centred(key_of[11], (EXPERTS, D, FF), D ** -0.5, 0.125, ((0, 8), (2, 4)))
    down_weight = centred(key_of[12], (EXPERTS, FF, D), FF ** -0.5, 0.1875, ((0, 8), (1, 4)))
    return dict(query_rows=query_rows, key_rows=key_rows, retrieved_vector_table=retrieved_vector_table, key_bias=key_bias, score_offset=score_offset, out_weight=out_weight, second_batch_activations=second_batch_activations, norm_gain=norm_gain, expert_index=expert_index, route_weight=route_weight, gate_weight=gate_weight, up_weight=up_weight, down_weight=down_weight)


def block_terms(query_block, key_block, value_block, bias_block, offset, causal_mask):
    scale = 1.0 / math.sqrt(query_block.shape[-1])
    scores = jnp.einsum('tkgd,skd->kgts', query_block.astype(jnp.float32), key_block.astype(jnp.float32)) * scale
    scores = scores + jnp.transpose(bias_block.astype(jnp.float32))[:, None, None, :] - offset[:, :, None, None]
    length = query_block.shape[0]
    if causal_mask:
        later = lax.broadcasted_iota(jnp.int32, (length, length), 0) > lax.broadcasted_iota(jnp.int32, (length, length), 1)
        keep = jnp.where(later, jax.nn.log_sigmoid(-scores), 0.0)
        suffix = lax.cumsum(keep, axis=3, reverse=True) - keep
        weight = jnp.where(later, jnp.exp(jax.nn.log_sigmoid(scores) + suffix), 0.0)
    else:
        keep = jax.nn.log_sigmoid(-scores)
        suffix = lax.cumsum(keep, axis=3, reverse=True) - keep
        weight = jnp.exp(jax.nn.log_sigmoid(scores) + suffix)
    weight = weight.astype(jnp.bfloat16)
    block_out = jnp.einsum('kgts,skd->kgtd', weight.astype(jnp.float32), value_block.astype(jnp.float32))
    return (block_out, lax.optimization_barrier(jnp.sum(keep, axis=3)))

def attention_half(query_rows, key_rows, retrieved_vector_table, key_bias, score_offset, out_weight):
    group = HEADS // KVH
    span = N_EP // SEQS
    blocks = query_rows.shape[0] // ROWS_A
    queries = query_rows.reshape(blocks, ROWS_A, KVH, group, HD)
    keyset = key_rows.reshape(blocks, ROWS_A, KVH, HD)
    valueset = retrieved_vector_table.reshape(blocks, ROWS_A, KVH, HD)
    biases = key_bias.reshape(blocks, ROWS_A, KVH)
    offset = score_offset.reshape(KVH, group)

    def one_block(block_index):
        query_block = queries[block_index]
        result, near = block_terms(query_block, keyset[block_index], valueset[block_index], biases[block_index], offset, True)
        first = block_index - block_index % span

        def step(distance, state):
            result, near = state
            source = block_index - distance
            block_out, total = block_terms(query_block, keyset[source], valueset[source], biases[source], offset, False)
            return (result + jnp.exp(near)[..., None] * block_out, near + total)
        result, near = lax.fori_loop(1, block_index - first + 1, step, (result, near))
        return result
    outs = lax.map(one_block, jnp.arange(blocks, dtype=jnp.int32))
    attended = jnp.transpose(outs, (0, 3, 1, 2, 4)).reshape(query_rows.shape[0], HEADS * HD).astype(jnp.bfloat16)
    width = attended.shape[1] // N_TP
    summed = jnp.zeros((attended.shape[0], out_weight.shape[1]), jnp.float32)
    for section in range(N_TP):
        product_terms = jnp.dot(attended[:, section * width:(section + 1) * width], out_weight[section * width:(section + 1) * width], preferred_element_type=jnp.float32)
        rounded = lax.optimization_barrier(product_terms.astype(jnp.bfloat16))
        summed = summed + rounded.astype(jnp.float32)
    return summed.astype(jnp.bfloat16)

def expert_half(second_batch_activations, norm_gain, expert_index, route_weight, gate_weight, up_weight, down_weight):
    values32 = second_batch_activations.astype(jnp.float32)
    normed = (values32 * lax.rsqrt(lax.optimization_barrier(jnp.mean(values32 * values32, axis=1, keepdims=True)) + 1e-06) * norm_gain).astype(jnp.bfloat16)
    flat = expert_index.reshape(-1)
    weights = route_weight.reshape(-1)
    limit = N_EP * CAP
    width = FF // N_TP

    def one_expert(summed, expert):
        chosen = jnp.nonzero(flat == expert, size=limit, fill_value=0)[0].astype(jnp.int32)
        count = jnp.sum((flat == expert).astype(jnp.int32))
        valid = jnp.arange(limit, dtype=jnp.int32) < count
        token = chosen // TOP
        rows = normed[token]
        gate_pre = jnp.dot(rows, gate_weight[expert], preferred_element_type=jnp.float32)
        up_pre = jnp.dot(rows, up_weight[expert], preferred_element_type=jnp.float32)
        hidden = (jax.nn.silu(gate_pre) * up_pre).astype(jnp.bfloat16)
        down = down_weight[expert]
        result = jnp.zeros((limit, D), jnp.float32)
        for section in range(N_TP):
            product_terms = jnp.dot(hidden[:, section * width:(section + 1) * width], down[section * width:(section + 1) * width], preferred_element_type=jnp.float32)
            rounded = lax.optimization_barrier(product_terms.astype(jnp.bfloat16))
            result = result + rounded.astype(jnp.float32)
        result = result.astype(jnp.bfloat16).astype(jnp.float32)
        scale = jnp.where(valid, weights[chosen], 0.0)
        return (summed.at[token].add(scale[:, None] * result), None)
    summed, unused = lax.scan(one_expert, jnp.zeros((second_batch_activations.shape[0], D), jnp.float32), jnp.arange(EXPERTS, dtype=jnp.int32))
    return summed.astype(jnp.bfloat16)

def reference(query_rows, key_rows, retrieved_vector_table, key_bias, score_offset, out_weight, second_batch_activations, norm_gain, expert_index, route_weight, gate_weight, up_weight, down_weight):
    attention_out = attention_half(query_rows, key_rows, retrieved_vector_table, key_bias, score_offset, out_weight)
    expert_out = expert_half(second_batch_activations, norm_gain, expert_index, route_weight, gate_weight, up_weight, down_weight)
    return (attention_out, expert_out)
```

```python
import functools
import math

import jax
import jax.numpy as jnp
from jax import lax
from jax.experimental import pallas as pl
from jax.experimental.pallas import tpu as pltpu
from jax.sharding import PartitionSpec as P

HD = 64
SEQS = 1
GROUPS = 4
F32 = jnp.float32
BF16 = jnp.bfloat16
MESH = pl.DeviceIdType.MESH


def dot(a, b):
    return jnp.dot(a, b, preferred_element_type=F32)


def kernel(
    n, ntp, cap, heads,
    q_ref, k_ref, v_ref, bias_ref, off_ref, wo_hbm, x_ref, gain_ref, idx_ref, rw_ref,
    wg_hbm, wu_hbm, wd_hbm,
    att_out, exp_out,
    kvb, kvs, q4, acc, near, wgu, wd, wo, comb_t, rwt_t, wt, sendx, xs,
    send_a, recv_a, own, send_b, recv_b, res, ret, att_send, att_recv,
    wsem, kv_ss, kv_rs, dx_ss, dx_rs, cr_ss, cr_rs, pa_ss, pa_rs, fw_ss, fw_rs,
    a_ss, a_rs, b_ss, b_rs, r_ss, r_rs, o_ss, o_rs,
):
    me = lax.axis_index("ep")
    tp = lax.axis_index("tp")
    rows = q_ref.shape[0]
    quarter = x_ref.shape[1] // ntp
    ff = wd.shape[0]
    span = n // SEQS
    place = lax.rem(me, span)
    mate = tp + 1 - 2 * lax.rem(tp, 2)
    across = lax.rem(tp + 2, ntp)
    mate_across = lax.rem(mate + 2, ntp)

    barrier = pltpu.get_barrier_semaphore()
    for d in range(1, n):
        pl.semaphore_signal(barrier, inc=1, device_id={"ep": lax.rem(me + d, n)}, device_id_type=MESH)
    for j in range(1, ntp):
        pl.semaphore_signal(barrier, inc=1, device_id={"tp": lax.rem(tp + j, ntp)}, device_id_type=MESH)

    loads = [
        pltpu.make_async_copy(wg_hbm.at[0], wgu.at[:, pl.ds(0, ff)], wsem.at[0]),
        pltpu.make_async_copy(wu_hbm.at[0], wgu.at[:, pl.ds(ff, ff)], wsem.at[1]),
        pltpu.make_async_copy(wd_hbm.at[0], wd, wsem.at[2]),
        pltpu.make_async_copy(wo_hbm, wo, wsem.at[3]),
    ]
    for load in loads:
        load.start()

    def part(d):
        return pl.ds(pl.multiple_of(d * cap, cap), cap)

    def remote(src, dst, ss, rs, where):
        return pltpu.make_async_remote_copy(
            src_ref=src, dst_ref=dst, send_sem=ss, recv_sem=rs, device_id=where, device_id_type=MESH
        )

    def kv_copy(d):
        return remote(kvs, kvb.at[d], kv_ss.at[d], kv_rs.at[d], {"ep": lax.rem(me + d, n)})

    def dx_copy(d):
        return remote(
            sendx.at[part(d)], xs.at[tp, part(d)], dx_ss.at[d], dx_rs.at[d], {"ep": lax.rem(me + d, n)}
        )

    def cross_send(d):
        return remote(xs.at[tp, part(d)], xs.at[tp, part(d)], cr_ss.at[d], cr_rs.at[d], {"tp": across})

    def cross_recv(d):
        return remote(xs.at[across, part(d)], xs.at[across, part(d)], cr_ss.at[d], cr_rs.at[d], {"tp": across})

    def mate_send(d):
        return remote(xs.at[tp, part(d)], xs.at[tp, part(d)], pa_ss.at[d], pa_rs.at[d], {"tp": mate})

    def mate_recv(d):
        return remote(xs.at[mate, part(d)], xs.at[mate, part(d)], pa_ss.at[d], pa_rs.at[d], {"tp": mate})

    def fwd_send(d):
        return remote(xs.at[across, part(d)], xs.at[across, part(d)], fw_ss.at[d], fw_rs.at[d], {"tp": mate})

    def fwd_recv(d):
        return remote(
            xs.at[mate_across, part(d)], xs.at[mate_across, part(d)], fw_ss.at[d], fw_rs.at[d], {"tp": mate}
        )

    kvs[0:rows, :] = jnp.concatenate([k_ref[...], v_ref[...]], axis=1)
    bias_square = jnp.broadcast_to(bias_ref[...].astype(F32), (rows, 128))
    kvs[rows : rows + 16, :] = jnp.transpose(bias_square)[0:16, :].astype(BF16)

    lane = lax.broadcasted_iota(jnp.int32, (rows, 128), 1)
    sub = lax.broadcasted_iota(jnp.int32, (rows, 128), 0)
    first = jnp.where(idx_ref[:, 0:1] == lane, 1.0, 0.0).astype(F32)
    second = jnp.where(idx_ref[:, 1:2] == lane, 1.0, 0.0).astype(F32)
    member = first + second
    below = jnp.where(sub > lane, 1.0, 0.0).astype(F32).astype(BF16)
    slot = dot(below, member.astype(BF16))
    comb_t[...] = jnp.transpose(jnp.where(member > 0.5, slot, -1.0))
    rwt_t[...] = jnp.transpose(first * rw_ref[:, 0:1] + second * rw_ref[:, 1:2])

    x32 = x_ref[...].astype(F32)
    inverse = lax.rsqrt(jnp.mean(x32 * x32, axis=1, keepdims=True) + 1e-06)
    columns = pl.ds(pl.multiple_of(tp * quarter, quarter), quarter)
    normed = (x_ref[:, columns].astype(F32) * inverse * gain_ref[:, columns]).astype(BF16)

    pl.semaphore_wait(barrier, n - 1 + ntp - 1)

    for d in range(1, n):
        @pl.when(place + d < span)
        def _(d=d):
            kv_copy(d).start()

    slot_iota = lax.broadcasted_iota(jnp.int32, (cap, 128), 0).astype(F32)
    for step in range(n):
        d = (step + 1) % n
        e = lax.rem(me + d, n)
        hit = comb_t[pl.ds(e, 1), :] == slot_iota
        wt[d * cap : (d + 1) * cap, :] = jnp.where(hit, rwt_t[pl.ds(e, 1), :], 0.0).astype(BF16)
        picked = dot(jnp.where(hit, 1.0, 0.0).astype(BF16), normed).astype(BF16)
        if d:
            sendx[d * cap : (d + 1) * cap, :] = picked
            dx_copy(d).start()
        else:
            xs[tp, 0:cap, :] = picked
    cross_send(0).start()
    mate_send(0).start()

    strict = jnp.where(sub > lane, 1.0, 0.0).astype(F32).astype(BF16)
    strict2 = jnp.concatenate([strict, strict], axis=0)
    later = sub > lane
    for h in range(heads):
        piece = q_ref[:, h * HD : (h + 1) * HD].astype(F32) * (1.0 / math.sqrt(HD))
        q4[h * rows : (h + 1) * rows, :] = jnp.concatenate(
            [piece, jnp.zeros((rows, 128 - HD), F32)], axis=1
        ).astype(BF16)

    def block(kv_ref, diagonal):
        kv = kv_ref[0:rows, :]
        bias = kv_ref[rows : rows + 16, :].astype(F32)[0:1, :]
        for h in range(heads):
            hs = slice(h * rows, (h + 1) * rows)
            score = lax.dot_general(
                q4[hs, :], kv, (((1,), (1,)), ((), ())), preferred_element_type=F32
            ) + (bias - off_ref[h])
            drop = jnp.maximum(score, 0.0) + jnp.log(1.0 + jnp.exp(-jnp.abs(score)))
            own_log = score - drop
            if diagonal:
                drop = jnp.where(later, drop, 0.0)
            high = drop.astype(BF16)
            low = (drop - high.astype(F32)).astype(BF16)
            after = dot(jnp.concatenate([high, low], axis=1), strict2)
            weight = jnp.exp(own_log - after)
            if diagonal:
                weight = jnp.where(later, weight, 0.0)
            out = dot(weight.astype(BF16), kv)
            total = jnp.broadcast_to(after[:, 0:1] + drop[:, 0:1], (rows, 128))
            if diagonal:
                acc[hs, :] = out
                near[hs, :] = total
            else:
                acc[hs, :] = acc[hs, :] + jnp.exp(-near[hs, :]) * out
                near[hs, :] = near[hs, :] + total

    block(kvs, True)

    def step_of(i, carry):
        dx_copy(i).wait_recv()
        cross_send(i).start()
        mate_send(i).start()
        cross_recv(i - 1).wait_recv()
        fwd_send(i - 1).start()

        @pl.when(place - i >= 0)
        def _():
            kv_copy(i).wait_recv()
            block(kvb.at[i], False)

        return carry

    lax.fori_loop(1, n, step_of, 0)
    cross_recv(n - 1).wait_recv()
    fwd_send(n - 1).start()

    loads[3].wait()
    attended = jnp.concatenate(
        [acc[h * rows : (h + 1) * rows, :][:, HD : 2 * HD] for h in range(heads)], axis=1
    ).astype(BF16)
    att_send[...] = dot(attended, wo[...]).astype(BF16)
    band = rows // ntp

    def att_copy(j):
        peer = lax.rem(tp + j, ntp)
        return remote(
            att_send.at[pl.ds(pl.multiple_of(peer * band, band), band)], att_recv.at[j],
            o_ss.at[j], o_rs.at[j], {"tp": peer},
        )

    for j in range(1, ntp):
        att_copy(j).start()

    for load in loads[0:3]:
        load.wait()
    per = n // GROUPS
    size = per * cap

    def a_copy(g):
        gs = pl.ds(g * size, size)
        return remote(send_a.at[:, gs], recv_a.at[:, gs], a_ss.at[g], a_rs.at[g], {"tp": mate})

    def b_copy(g):
        gs = pl.ds(g * size, size)
        return remote(send_b.at[gs], recv_b.at[gs], b_ss.at[g], b_rs.at[g], {"tp": across})

    def r_copy(d):
        return remote(
            res.at[part(d)], ret.at[part(d)], r_ss.at[d], r_rs.at[d], {"ep": lax.rem(me - d + n, n)}
        )

    def wd_part(q):
        return wd[:, pl.ds(pl.multiple_of(q * quarter, quarter), quarter)]

    for t in range(GROUPS + 2):
        if t < GROUPS:
            gs = slice(t * size, (t + 1) * size)
            for d in range(t * per, (t + 1) * per):
                mate_recv(d).wait_recv()
                fwd_recv(d).wait_recv()
            both = dot(xs[0, gs, :], wgu[0:quarter, :])
            for q in range(1, ntp):
                both = both + dot(xs[q, gs, :], wgu[q * quarter : (q + 1) * quarter, :])
            gate = both[:, 0:ff]
            hidden = (gate / (1.0 + jnp.exp(-gate)) * both[:, ff : 2 * ff]).astype(BF16)
            send_a[0, gs, :] = dot(hidden, wd_part(mate)).astype(BF16)
            send_a[1, gs, :] = dot(hidden, wd_part(mate_across)).astype(BF16)
            a_copy(t).start()
            own[0, gs, :] = dot(hidden, wd_part(tp))
            own[1, gs, :] = dot(hidden, wd_part(across))
        if 1 <= t <= GROUPS:
            g = t - 1
            gs = slice(g * size, (g + 1) * size)
            a_copy(g).wait_recv()
            send_b[gs, :] = (own[1, gs, :] + recv_a[1, gs, :].astype(F32)).astype(BF16)
            b_copy(g).start()
        if t >= 2:
            g = t - 2
            gs = slice(g * size, (g + 1) * size)
            b_copy(g).wait_recv()
            final = (
                own[0, gs, :] + recv_a[0, gs, :].astype(F32) + recv_b[gs, :].astype(F32)
            ).astype(BF16)
            res[gs, :] = final
            for d in range(g * per, (g + 1) * per):
                if d:
                    r_copy(d).start()
            if g == 0:
                ret[0:cap, :] = final[0:cap, :]

    for j in range(1, ntp):
        att_copy(j).wait_recv()
    summed = att_send[pl.ds(pl.multiple_of(tp * band, band), band), :].astype(F32)
    for j in range(1, ntp):
        summed = summed + att_recv[j].astype(F32)
    att_out[...] = summed.astype(BF16)

    for d in range(1, n):
        r_copy(d).wait_recv()
    exp_out[...] = lax.dot_general(
        wt[...], ret[...], (((0,), (0,)), ((), ())), preferred_element_type=F32
    ).astype(BF16)

    for d in range(1, n):
        @pl.when(place + d < span)
        def _(d=d):
            kv_copy(d).wait_send()

        dx_copy(d).wait_send()
        r_copy(d).wait_send()
    for d in range(n):
        cross_send(d).wait_send()
        mate_send(d).wait_send()
        fwd_send(d).wait_send()
    for g in range(GROUPS):
        a_copy(g).wait_send()
        b_copy(g).wait_send()
    for j in range(1, ntp):
        att_copy(j).wait_send()


def body(n, ntp, q, k, v, bias, off, wo, x, gain, idx, rw, wg, wu, wd):
    rows, tokens, width = q.shape[0], x.shape[0], x.shape[1]
    heads = q.shape[1] // HD
    cap = max(16, -(-2 * tokens * idx.shape[1] // n // 16) * 16)
    total = n * cap
    quarter = width // ntp
    ff = wd.shape[1]
    band = rows // ntp
    vmem = pl.BlockSpec(memory_space=pltpu.VMEM)
    anyspace = pl.BlockSpec(memory_space=pl.ANY)
    smem = pl.BlockSpec(memory_space=pltpu.SMEM)
    dma = pltpu.SemaphoreType.DMA
    return pl.pallas_call(
        functools.partial(kernel, n, ntp, cap, heads),
        out_shape=(
            jax.ShapeDtypeStruct((band, wo.shape[1]), BF16),
            jax.ShapeDtypeStruct((tokens, quarter), BF16),
        ),
        in_specs=[vmem, vmem, vmem, vmem, smem, anyspace, vmem, vmem, vmem, vmem, anyspace, anyspace, anyspace],
        out_specs=(vmem, vmem),
        scratch_shapes=[
            pltpu.VMEM((n, rows + 16, 128), BF16),
            pltpu.VMEM((rows + 16, 128), BF16),
            pltpu.VMEM((heads * rows, 128), BF16),
            pltpu.VMEM((heads * rows, 128), F32),
            pltpu.VMEM((heads * rows, 128), F32),
            pltpu.VMEM((width, 2 * ff), BF16),
            pltpu.VMEM((ff, width), BF16),
            pltpu.VMEM(wo.shape, BF16),
            pltpu.VMEM((128, tokens), F32),
            pltpu.VMEM((128, tokens), F32),
            pltpu.VMEM((total, tokens), BF16),
            pltpu.VMEM((total, quarter), BF16),
            pltpu.VMEM((ntp, total, quarter), BF16),
            pltpu.VMEM((2, total, quarter), BF16),
            pltpu.VMEM((2, total, quarter), BF16),
            pltpu.VMEM((2, total, quarter), F32),
            pltpu.VMEM((total, quarter), BF16),
            pltpu.VMEM((total, quarter), BF16),
            pltpu.VMEM((total, quarter), BF16),
            pltpu.VMEM((total, quarter), BF16),
            pltpu.VMEM((rows, wo.shape[1]), BF16),
            pltpu.VMEM((ntp, band, wo.shape[1]), BF16),
            dma((4,)),
        ]
        + [dma((n,))] * 10
        + [dma((GROUPS,))] * 4
        + [dma((n,))] * 2
        + [dma((ntp,))] * 2,
        compiler_params=pltpu.CompilerParams(collective_id=0, has_side_effects=True),
    )(q, k, v, bias, off, wo, x, gain.reshape(1, -1), idx, rw, wg, wu, wd)


def solution(mesh):
    return jax.shard_map(
        functools.partial(body, mesh.shape["ep"], mesh.shape["tp"]),
        mesh=mesh,
        in_specs=(
            P("ep", "tp"),
            P("ep", "tp"),
            P("ep", "tp"),
            P("ep", "tp"),
            P("tp"),
            P("tp", None),
            P("ep", None),
            P(),
            P("ep", None),
            P("ep", None),
            P("ep", None, "tp"),
            P("ep", None, "tp"),
            P("ep", "tp", None),
        ),
        out_specs=(P(("ep", "tp"), None), P("ep", "tp")),
        check_vma=False,
    )
```

```python
import functools
import math

import jax
import jax.numpy as jnp
from jax import lax
from jax.experimental import pallas as pl
from jax.experimental.pallas import tpu as pltpu
from jax.sharding import PartitionSpec as P

HD = 64
SEQS = 1
GROUPS = 4
F32 = jnp.float32
BF16 = jnp.bfloat16
MESH = pl.DeviceIdType.MESH


def dot(a, b):
    return jnp.dot(a, b, preferred_element_type=F32)


def kernel(
    n, ntp, cap, heads,
    q_ref, k_ref, v_ref, bias_ref, off_ref, wo_hbm, x_ref, gain_ref, idx_ref, rw_ref,
    wg_hbm, wu_hbm, wd_hbm,
    att_out, exp_out,
    kvb, kvs, q4, acc, near, wgu, wd, wo, comb_t, rwt_t, wt, sendx, xs,
    send_a, recv_a, own, send_b, recv_b, res, ret, att_send, att_recv,
    wsem, kv_ss, kv_rs, dx_ss, dx_rs, cr_ss, cr_rs, pa_ss, pa_rs, fw_ss, fw_rs,
    a_ss, a_rs, b_ss, b_rs, r_ss, r_rs, o_ss, o_rs,
):
    me = lax.axis_index("ep")
    tp = lax.axis_index("tp")
    rows = q_ref.shape[0]
    quarter = x_ref.shape[1] // ntp
    ff = wd.shape[0]
    span = n // SEQS
    place = lax.rem(me, span)
    mate = tp + 1 - 2 * lax.rem(tp, 2)
    across = lax.rem(tp + 2, ntp)
    mate_across = lax.rem(mate + 2, ntp)

    barrier = pltpu.get_barrier_semaphore()
    for d in range(1, n):
        pl.semaphore_signal(barrier, inc=1, device_id={"ep": lax.rem(me + d, n)}, device_id_type=MESH)
    for j in range(1, ntp):
        pl.semaphore_signal(barrier, inc=1, device_id={"tp": lax.rem(tp + j, ntp)}, device_id_type=MESH)

    loads = [
        pltpu.make_async_copy(wg_hbm.at[0], wgu.at[:, pl.ds(0, ff)], wsem.at[0]),
        pltpu.make_async_copy(wu_hbm.at[0], wgu.at[:, pl.ds(ff, ff)], wsem.at[1]),
        pltpu.make_async_copy(wd_hbm.at[0], wd, wsem.at[2]),
        pltpu.make_async_copy(wo_hbm, wo, wsem.at[3]),
    ]
    for load in loads:
        load.start()

    def part(d):
        return pl.ds(pl.multiple_of(d * cap, cap), cap)

    def remote(src, dst, ss, rs, where):
        return pltpu.make_async_remote_copy(
            src_ref=src, dst_ref=dst, send_sem=ss, recv_sem=rs, device_id=where, device_id_type=MESH
        )

    def kv_copy(d):
        return remote(kvs, kvb.at[d], kv_ss.at[d], kv_rs.at[d], {"ep": lax.rem(me + d, n)})

    def dx_copy(d):
        return remote(
            sendx.at[part(d)], xs.at[tp, part(d)], dx_ss.at[d], dx_rs.at[d], {"ep": lax.rem(me + d, n)}
        )

    def cross_send(d):
        return remote(xs.at[tp, part(d)], xs.at[tp, part(d)], cr_ss.at[d], cr_rs.at[d], {"tp": across})

    def cross_recv(d):
        return remote(xs.at[across, part(d)], xs.at[across, part(d)], cr_ss.at[d], cr_rs.at[d], {"tp": across})

    def mate_send(d):
        return remote(xs.at[tp, part(d)], xs.at[tp, part(d)], pa_ss.at[d], pa_rs.at[d], {"tp": mate})

    def mate_recv(d):
        return remote(xs.at[mate, part(d)], xs.at[mate, part(d)], pa_ss.at[d], pa_rs.at[d], {"tp": mate})

    def fwd_send(d):
        return remote(xs.at[across, part(d)], xs.at[across, part(d)], fw_ss.at[d], fw_rs.at[d], {"tp": mate})

    def fwd_recv(d):
        return remote(
            xs.at[mate_across, part(d)], xs.at[mate_across, part(d)], fw_ss.at[d], fw_rs.at[d], {"tp": mate}
        )

    kvs[0:HD, :] = k_ref[...]
    kvs[HD : 2 * HD, :] = v_ref[...]
    kvs[2 * HD : 2 * HD + 16, :] = jnp.broadcast_to(bias_ref[...].astype(F32), (16, rows)).astype(BF16)

    lane = lax.broadcasted_iota(jnp.int32, (128, rows), 1)
    sub = lax.broadcasted_iota(jnp.int32, (128, rows), 0)
    first = jnp.where(idx_ref[0:1, :] == sub, 1.0, 0.0).astype(F32)
    second = jnp.where(idx_ref[1:2, :] == sub, 1.0, 0.0).astype(F32)
    member = first + second
    above = jnp.where(sub < lane, 1.0, 0.0).astype(F32).astype(BF16)
    slot = dot(member.astype(BF16), above)
    comb_t[...] = jnp.where(member > 0.5, slot, -1.0)
    rwt_t[...] = first * rw_ref[0:1, :] + second * rw_ref[1:2, :]

    x32 = x_ref[...].astype(F32)
    inverse = lax.rsqrt(jnp.mean(x32 * x32, axis=1, keepdims=True) + 1e-06)
    columns = pl.ds(pl.multiple_of(tp * quarter, quarter), quarter)
    normed = (x_ref[:, columns].astype(F32) * inverse * gain_ref[:, columns]).astype(BF16)

    pl.semaphore_wait(barrier, n - 1 + ntp - 1)

    slot_iota = lax.broadcasted_iota(jnp.int32, (cap, 128), 0).astype(F32)
    for step in range(n):
        d = step
        e = lax.rem(me + d, n)
        hit = comb_t[pl.ds(e, 1), :] == slot_iota
        wt[d * cap : (d + 1) * cap, :] = jnp.where(hit, rwt_t[pl.ds(e, 1), :], 0.0).astype(BF16)
        picked = dot(jnp.where(hit, 1.0, 0.0).astype(BF16), normed).astype(BF16)
        if d:
            sendx[d * cap : (d + 1) * cap, :] = picked
            dx_copy(d).start()
        else:
            xs[tp, 0:cap, :] = picked
            cross_send(0).start()
            mate_send(0).start()
    for d in range(1, n):
        @pl.when(place + d < span)
        def _(d=d):
            kv_copy(d).start()


    strict = jnp.where(sub > lane, 1.0, 0.0).astype(F32).astype(BF16)
    strict2 = jnp.concatenate([strict, strict], axis=0)
    later = sub > lane
    for h in range(heads):
        piece = q_ref[:, h * HD : (h + 1) * HD].astype(F32) * (1.0 / math.sqrt(HD))
        q4[h * rows : (h + 1) * rows, :] = jnp.concatenate(
            [piece, jnp.zeros((rows, 128 - HD), F32)], axis=1
        ).astype(BF16)

    def block(kv_ref, diagonal):
        kv = kv_ref[0 : 2 * HD, :]
        bias = kv_ref[2 * HD : 2 * HD + 16, :].astype(F32)[0:1, :]
        for h in range(heads):
            hs = slice(h * rows, (h + 1) * rows)
            score = dot(q4[hs, :], kv) + (bias - off_ref[h])
            drop = jnp.maximum(score, 0.0) + jnp.log(1.0 + jnp.exp(-jnp.abs(score)))
            own_log = score - drop
            if diagonal:
                drop = jnp.where(later, drop, 0.0)
            high = drop.astype(BF16)
            low = (drop - high.astype(F32)).astype(BF16)
            after = dot(jnp.concatenate([high, low], axis=1), strict2)
            weight = jnp.exp(own_log - after)
            if diagonal:
                weight = jnp.where(later, weight, 0.0)
            out = lax.dot_general(
                weight.astype(BF16), kv, (((1,), (1,)), ((), ())), preferred_element_type=F32
            )
            total = jnp.broadcast_to(after[:, 0:1] + drop[:, 0:1], (rows, 128))
            if diagonal:
                acc[hs, :] = out
                near[hs, :] = total
            else:
                acc[hs, :] = acc[hs, :] + jnp.exp(-near[hs, :]) * out
                near[hs, :] = near[hs, :] + total

    block(kvs, True)

    def step_of(i, carry):
        @pl.when(place - i >= 0)
        def _():
            kv_copy(i).wait_recv()
            block(kvb.at[i], False)

        return carry

    band = rows // ntp

    def att_copy(j):
        peer = lax.rem(tp + j, ntp)
        return remote(
            att_send.at[pl.ds(pl.multiple_of(peer * band, band), band)], att_recv.at[j],
            o_ss.at[j], o_rs.at[j], {"tp": peer},
        )

    for load in loads[0:3]:
        load.wait()
    per = n // GROUPS
    size = per * cap

    def a_copy(g):
        gs = pl.ds(g * size, size)
        return remote(send_a.at[:, gs], recv_a.at[:, gs], a_ss.at[g], a_rs.at[g], {"tp": mate})

    def b_copy(g):
        gs = pl.ds(g * size, size)
        return remote(send_b.at[gs], recv_b.at[gs], b_ss.at[g], b_rs.at[g], {"tp": across})

    def r_copy(d):
        return remote(
            res.at[part(d)], ret.at[part(d)], r_ss.at[d], r_rs.at[d], {"ep": lax.rem(me - d + n, n)}
        )

    def wd_part(q):
        return wd[:, pl.ds(pl.multiple_of(q * quarter, quarter), quarter)]

    def collect(g):
        for d in range(max(1, g * per), (g + 1) * per):
            dx_copy(d).wait_recv()
            cross_send(d).start()
            mate_send(d).start()

    def forward(g):
        for d in range(g * per, (g + 1) * per):
            cross_recv(d).wait_recv()
            fwd_send(d).start()

    def expert(g):
        gs = slice(g * size, (g + 1) * size)
        for d in range(g * per, (g + 1) * per):
            mate_recv(d).wait_recv()
            fwd_recv(d).wait_recv()
        both = dot(xs[0, gs, :], wgu[0:quarter, :])
        for q in range(1, ntp):
            both = both + dot(xs[q, gs, :], wgu[q * quarter : (q + 1) * quarter, :])
        gate = both[:, 0:ff]
        hidden = (gate / (1.0 + jnp.exp(-gate)) * both[:, ff : 2 * ff]).astype(BF16)
        send_a[1, gs, :] = dot(hidden, wd_part(mate_across)).astype(BF16)
        send_a[0, gs, :] = dot(hidden, wd_part(mate)).astype(BF16)
        a_copy(g).start()
        own[1, gs, :] = dot(hidden, wd_part(across))
        own[0, gs, :] = dot(hidden, wd_part(tp))

    def reduce_near(g):
        gs = slice(g * size, (g + 1) * size)
        a_copy(g).wait_recv()
        send_b[gs, :] = (own[1, gs, :] + recv_a[1, gs, :].astype(F32)).astype(BF16)
        b_copy(g).start()

    def give_back(g):
        gs = slice(g * size, (g + 1) * size)
        b_copy(g).wait_recv()
        final = (own[0, gs, :] + recv_a[0, gs, :].astype(F32) + recv_b[gs, :].astype(F32)).astype(BF16)
        res[gs, :] = final
        for d in range(max(1, g * per), (g + 1) * per):
            r_copy(d).start()
        if g == 0:
            ret[0:cap, :] = final[0:cap, :]

    for t in range(GROUPS + 2):
        if t < GROUPS:
            collect(t)
        if 1 <= t <= GROUPS:
            forward(t - 1)
        if 2 <= t:
            reduce_near(t - 2)
        if 3 <= t:
            give_back(t - 3)
        if 1 <= t <= GROUPS:
            expert(t - 1)

    lax.fori_loop(1, n, step_of, 0)
    loads[3].wait()
    attended = jnp.concatenate(
        [acc[h * rows : (h + 1) * rows, :][:, HD : 2 * HD] for h in range(heads)], axis=1
    ).astype(BF16)
    att_send[...] = dot(attended, wo[...]).astype(BF16)
    for j in range(1, ntp):
        att_copy(j).start()

    give_back(GROUPS - 1)

    for j in range(1, ntp):
        att_copy(j).wait_recv()
    summed = att_send[pl.ds(pl.multiple_of(tp * band, band), band), :].astype(F32)
    for j in range(1, ntp):
        summed = summed + att_recv[j].astype(F32)
    att_out[...] = summed.astype(BF16)

    for d in range(1, n):
        r_copy(d).wait_recv()
    exp_out[...] = lax.dot_general(
        wt[...], ret[...], (((0,), (0,)), ((), ())), preferred_element_type=F32
    ).astype(BF16)

    for d in range(1, n):
        @pl.when(place + d < span)
        def _(d=d):
            kv_copy(d).wait_send()

        dx_copy(d).wait_send()
        r_copy(d).wait_send()
    for d in range(n):
        cross_send(d).wait_send()
        mate_send(d).wait_send()
        fwd_send(d).wait_send()
    for g in range(GROUPS):
        a_copy(g).wait_send()
        b_copy(g).wait_send()
    for j in range(1, ntp):
        att_copy(j).wait_send()


def body(n, ntp, q, k, v, bias, off, wo, x, gain, idx, rw, wg, wu, wd):
    rows, tokens, width = q.shape[0], x.shape[0], x.shape[1]
    heads = q.shape[1] // HD
    cap = max(16, -(-2 * tokens * idx.shape[1] // n // 16) * 16)
    total = n * cap
    quarter = width // ntp
    ff = wd.shape[1]
    band = rows // ntp
    vmem = pl.BlockSpec(memory_space=pltpu.VMEM)
    anyspace = pl.BlockSpec(memory_space=pl.ANY)
    smem = pl.BlockSpec(memory_space=pltpu.SMEM)
    dma = pltpu.SemaphoreType.DMA
    return pl.pallas_call(
        functools.partial(kernel, n, ntp, cap, heads),
        out_shape=(
            jax.ShapeDtypeStruct((band, wo.shape[1]), BF16),
            jax.ShapeDtypeStruct((tokens, quarter), BF16),
        ),
        in_specs=[vmem, vmem, vmem, vmem, smem, anyspace, vmem, vmem, vmem, vmem, anyspace, anyspace, anyspace],
        out_specs=(vmem, vmem),
        scratch_shapes=[
            pltpu.VMEM((n, 2 * HD + 16, rows), BF16),
            pltpu.VMEM((2 * HD + 16, rows), BF16),
            pltpu.VMEM((heads * rows, 128), BF16),
            pltpu.VMEM((heads * rows, 128), F32),
            pltpu.VMEM((heads * rows, 128), F32),
            pltpu.VMEM((width, 2 * ff), BF16),
            pltpu.VMEM((ff, width), BF16),
            pltpu.VMEM(wo.shape, BF16),
            pltpu.VMEM((128, tokens), F32),
            pltpu.VMEM((128, tokens), F32),
            pltpu.VMEM((total, tokens), BF16),
            pltpu.VMEM((total, quarter), BF16),
            pltpu.VMEM((ntp, total, quarter), BF16),
            pltpu.VMEM((2, total, quarter), BF16),
            pltpu.VMEM((2, total, quarter), BF16),
            pltpu.VMEM((2, total, quarter), F32),
            pltpu.VMEM((total, quarter), BF16),
            pltpu.VMEM((total, quarter), BF16),
            pltpu.VMEM((total, quarter), BF16),
            pltpu.VMEM((total, quarter), BF16),
            pltpu.VMEM((rows, wo.shape[1]), BF16),
            pltpu.VMEM((ntp, band, wo.shape[1]), BF16),
            dma((4,)),
        ]
        + [dma((n,))] * 10
        + [dma((GROUPS,))] * 4
        + [dma((n,))] * 2
        + [dma((ntp,))] * 2,
        compiler_params=pltpu.CompilerParams(collective_id=0, has_side_effects=True),
    )(q, k.T, v.T, bias.T, off, wo, x, gain.reshape(1, -1), idx.T, rw.T, wg, wu, wd)


def solution(mesh):
    return jax.shard_map(
        functools.partial(body, mesh.shape["ep"], mesh.shape["tp"]),
        mesh=mesh,
        in_specs=(
            P("ep", "tp"),
            P("ep", "tp"),
            P("ep", "tp"),
            P("ep", "tp"),
            P("tp"),
            P("tp", None),
            P("ep", None),
            P(),
            P("ep", None),
            P("ep", None),
            P("ep", None, "tp"),
            P("ep", None, "tp"),
            P("ep", "tp", None),
        ),
        out_specs=(P(("ep", "tp"), None), P("ep", "tp")),
        check_vma=False,
    )
```
